1024 devices in a mesh: sp: 256 (over z, y, core), tp: 4 (over x).
Axes of the slice: x: 4, y: 8, z: 16, core: 2. Of those that a mesh axis runs over, the one named last changes fastest.
Arguments:
- tokens: bfloat16 [196608, 2048], P(('sp', 'tp')), may hold values from -6 to 6
- norm_gain: float32 [2048], replicated, may hold values from 0.1 to 1.9
- query_weight: bfloat16 [2048, 512], P(None, 'tp'), may hold values from -4 to 4
- key_weight: bfloat16 [2048, 256], P(None, 'tp'), may hold values from -4 to 4
- value_weight: bfloat16 [2048, 256], P(None, 'tp'), may hold values from -1 to 1
- sink_logit: float32 [8], P('tp'), may hold values from 2 to 6
- conv_gate_weight: bfloat16 [2048, 512], P(None, 'tp'), may hold values from -0.125 to 0.125
- conv_pre_weight: bfloat16 [2048, 512], P(None, 'tp'), may hold values from -0.125 to 0.125
- conv_input_weight: bfloat16 [2048, 512], P(None, 'tp'), may hold values from -0.125 to 0.125
- conv_taps: float32 [3, 512], P(None, 'tp'), may hold values from -3.5 to 3.5
- out_weight: bfloat16 [1024, 2048], replicated, may hold values from -0.1875 to 0.1875
Outputs:
- mixed: bfloat16 [196608, 2048], P(('sp', 'tp'))
The draws below stay inside these ranges and needn't reach their ends.
All inputs are finite; a program needn't handle non-finite values.
Results may differ from the reference program's by a relative error of at most 0.009.
Values may be sent and summed in bfloat16 or wider, within the bound.
No kernel may reach another device: no remote copies, remote signals or barrier semaphores. Data moves between devices by JAX's collectives and lax.ppermute only.
A program may use at most 32 MiB of HBM per device.

```python
import jax
import jax.numpy as jnp
from jax import lax

D = 2048
QH = 8
KVH = 4
HEAD_SIZE = 64
CW = 512
WIN = 128
TOK_DEV = 768
TOKENS = 196608
N_SP = 256


def draw_pair(key):
    base = jax.random.fold_in(key, 11)
    key_part = jax.random.normal(jax.random.fold_in(base, 1), (D, KVH * HEAD_SIZE), jnp.float32) * D ** (-0.5)
    noise_part = jax.random.normal(jax.random.fold_in(base, 2), (D, QH * HEAD_SIZE), jnp.float32) * D ** (-0.5)
    query_part = noise_part
    return (jnp.clip(query_part, -4.0, 4.0), jnp.clip(key_part, -4.0, 4.0))


def draw_query_weight(key, part):
    return draw_pair(key)[0].astype(jnp.bfloat16)


def draw_key_weight(key, part):
    return draw_pair(key)[1].astype(jnp.bfloat16)


def level_of(rng, extent, split, low, high):
    factor_of, own = 1.0, jax.random.fold_in(rng, 6)
    for position, blocks in split:
        draws = jnp.exp(jax.random.uniform(jax.random.fold_in(own, position), (blocks,), jnp.float32, low / len(split), high / len(split)))
        factor_of = factor_of * jnp.repeat(draws, extent[position] // blocks).reshape([-1 if axis == position else 1 for axis in range(len(extent))])
    return factor_of


def scatter_about(stream_key, extent, deviation, limit, split=(), held_as=jnp.bfloat16):
    array = deviation * jax.random.normal(stream_key, extent, jnp.float32)
    if split:
        array = array * level_of(stream_key, extent, split, -0.22, 0.18)
    return jnp.clip(array, -limit, limit).astype(held_as)


def setup_inputs(seed: int = 0) -> dict:
    key_list = jax.random.split(jax.random.key(seed), 12)
    return {
        "tokens": scatter_about(key_list[0], (TOKENS, D), 1.0, 6.0, ((0, 1024),)),
        "norm_gain": jnp.clip(1.0 + 0.18 * jax.random.normal(key_list[1], (D,), jnp.float32), 0.1, 1.9),
        "query_weight": draw_query_weight(jax.random.fold_in(key_list[11], 71), 0),
        "key_weight": draw_key_weight(jax.random.fold_in(key_list[11], 71), 0),
        "value_weight": scatter_about(key_list[4], (D, KVH * HEAD_SIZE), (D // 64) ** -0.5, 1.0, ((1, 4),)),
        "sink_logit": jnp.clip(2.0 + 4.0 * jax.random.uniform(key_list[5], (QH,), jnp.float32) ** level_of(key_list[5], (QH,), ((0, 4),), -0.2, 0.2), 2.0, 6.0),
        "conv_gate_weight": scatter_about(key_list[6], (D, CW), D ** -0.5, 0.125, ((1, 4),)),
        "conv_pre_weight": scatter_about(key_list[7], (D, CW), D ** -0.5, 0.125, ((1, 4),)),
        "conv_input_weight": scatter_about(key_list[8], (D, CW), D ** -0.5, 0.125, ((1, 4),)),
        "conv_taps": scatter_about(key_list[9], (3, CW), 3 ** -0.5, 3.5, ((1, 4),), jnp.float32),
        "out_weight": scatter_about(key_list[10], (QH * HEAD_SIZE + CW, D), (QH * HEAD_SIZE + CW) ** -0.5, 0.1875),
    }


def attend_block(query_block_tile, key_block_tile, value_block_tile, start, sinks, total):
    count = query_block_tile.shape[0]
    span = key_block_tile.shape[0]
    score_matrix = jnp.einsum('yxpz,ixz->xpyi', query_block_tile.astype(jnp.float32), key_block_tile.astype(jnp.float32)) * HEAD_SIZE ** (-0.5)
    query_pos = start + jnp.arange(count, dtype=jnp.int32)
    key_pos = start - WIN + jnp.arange(span, dtype=jnp.int32)
    valid = (jnp.abs(query_pos[:, None] - key_pos[None, :]) <= WIN) & (key_pos[None, :] >= 0) & (key_pos[None, :] < total)
    score_matrix = jnp.where(valid[None, None], score_matrix, -jnp.inf)
    sink_col = sinks.astype(jnp.float32)[:, :, None, None]
    top = jnp.maximum(lax.optimization_barrier(jnp.max(score_matrix, axis=-1, keepdims=True)), sink_col)
    expo = jnp.exp(score_matrix - top)
    denom = lax.optimization_barrier(jnp.sum(expo, axis=-1, keepdims=True)) + jnp.exp(sink_col - top)
    weight_lower_precision = (expo / denom).astype(jnp.bfloat16)
    final_output = jnp.einsum('bhcv,vbn->cbhn', weight_lower_precision.astype(jnp.float32), value_block_tile.astype(jnp.float32))
    return final_output.reshape(count, -1).astype(jnp.bfloat16)

def reference(tokens, norm_gain, query_weight, key_weight, value_weight, sink_logit, conv_gate_weight, conv_pre_weight, conv_input_weight, conv_taps, out_weight):
    tokens_f = tokens.astype(jnp.float32)
    normed = (tokens_f * lax.rsqrt(lax.optimization_barrier(jnp.mean(tokens_f * tokens_f, axis=-1, keepdims=True)) + 1e-06) * norm_gain).astype(jnp.bfloat16)
    queries = jnp.dot(normed, query_weight, preferred_element_type=jnp.float32).astype(jnp.bfloat16)
    key_rows = jnp.dot(normed, key_weight, preferred_element_type=jnp.float32).astype(jnp.bfloat16)
    value_rows = jnp.dot(normed, value_weight, preferred_element_type=jnp.float32).astype(jnp.bfloat16)
    ratio = QH // KVH
    total = TOKENS
    key_pad = jnp.pad(key_rows, ((WIN, WIN), (0, 0)))
    value_pad = jnp.pad(value_rows, ((WIN, WIN), (0, 0)))
    sinks = sink_logit.reshape(KVH, ratio)

    def one_block(index):
        start = (index * TOK_DEV).astype(jnp.int32)
        query_block_tile = lax.dynamic_slice_in_dim(queries, start, TOK_DEV, 0).reshape(TOK_DEV, KVH, ratio, HEAD_SIZE)
        key_block_tile = lax.dynamic_slice_in_dim(key_pad, start, TOK_DEV + 2 * WIN, 0).reshape(-1, KVH, HEAD_SIZE)
        value_block_tile = lax.dynamic_slice_in_dim(value_pad, start, TOK_DEV + 2 * WIN, 0).reshape(-1, KVH, HEAD_SIZE)
        return attend_block(query_block_tile, key_block_tile, value_block_tile, start, sinks, total)
    attended = lax.map(one_block, jnp.arange(N_SP, dtype=jnp.int32)).reshape(TOKENS, QH * HEAD_SIZE)
    conv_gate = jnp.dot(normed, conv_gate_weight, preferred_element_type=jnp.float32).astype(jnp.bfloat16)
    conv_pre = jnp.dot(normed, conv_pre_weight, preferred_element_type=jnp.float32).astype(jnp.bfloat16)
    conv_input = jnp.dot(normed, conv_input_weight, preferred_element_type=jnp.float32).astype(jnp.bfloat16)
    product = (conv_pre.astype(jnp.float32) * conv_input.astype(jnp.float32)).astype(jnp.bfloat16)
    padded = jnp.pad(product.astype(jnp.float32), ((1, 1), (0, 0)))
    convolved = conv_taps[0] * padded[:-2] + conv_taps[1] * padded[1:-1] + conv_taps[2] * padded[2:]
    conv_out = (conv_gate.astype(jnp.float32) * convolved).astype(jnp.bfloat16)
    joined = jnp.concatenate([attended, conv_out], axis=1)
    return jnp.dot(joined, out_weight, preferred_element_type=jnp.float32).astype(jnp.bfloat16)
```

```python
import jax
import jax.numpy as jnp
from jax import lax
from jax.experimental import pallas as pl
from jax.experimental.pallas import tpu as pltpu
from jax.sharding import PartitionSpec as P

HEAD = 64
WIN = 128
EDGE = 16
LANES = 128
F32 = jnp.float32
BF16 = jnp.bfloat16
VMEM = pl.BlockSpec(memory_space=pltpu.VMEM)
SMEM = pl.BlockSpec(memory_space=pltpu.SMEM)


def near_memory(*arrays):
    return tuple(pltpu.with_memory_space_constraint(array, pltpu.VMEM) for array in arrays)


def params(mebibytes):
    return pltpu.CompilerParams(vmem_limit_bytes=mebibytes << 20)


def split_kernel(tokens_ref, top_ref, bottom_ref, sems):
    half = top_ref.shape[0]
    copies = [
        pltpu.make_async_copy(tokens_ref.at[pl.ds(part * half, half)], ref, sems.at[part])
        for part, ref in enumerate((top_ref, bottom_ref))
    ]
    for copy in copies:
        copy.start()
    for copy in copies:
        copy.wait()


def pack_kernel(q_ref, k_ref, v_ref, gate_ref, pre_ref, input_ref, cols_ref, rows_ref):
    for place, ref in enumerate((q_ref, gate_ref, pre_ref, input_ref)):
        cols_ref[:, place * LANES : (place + 1) * LANES] = ref[...]
    for place, ref in enumerate((k_ref, k_ref, v_ref, v_ref)):
        rows_ref[place * HEAD : (place + 1) * HEAD, :] = ref[...]


def project(rows, gain, cols, kv_rows, out_ref, start):
    count = rows.shape[0]
    rows = rows.astype(F32)
    scale = lax.rsqrt(jnp.mean(rows * rows, axis=-1, keepdims=True) + 1e-06)
    normed = (rows * scale * gain).astype(BF16)
    out = jnp.dot(normed, cols, preferred_element_type=F32).astype(BF16)
    product = out[:, 2 * LANES : 3 * LANES].astype(F32) * out[:, 3 * LANES :].astype(F32)
    pairs = lax.dot_general(normed, kv_rows, (((1,), (1,)), ((), ())), preferred_element_type=F32)
    out_ref[pl.ds(start, count), : 2 * LANES] = out[:, : 2 * LANES]
    out_ref[pl.ds(start, count), 2 * LANES : 3 * LANES] = product.astype(BF16)
    out_ref[pl.ds(start, count), 3 * LANES :] = pairs.astype(BF16)


def near_kernel(top_ref, bottom_ref, at_ref, ab_ref, bt_ref, bb_ref, gain_ref, cols_ref, rows_ref, out_ref):
    gain, cols, rows = gain_ref[...], cols_ref[...], rows_ref[...]
    for place, ref in enumerate((top_ref, bottom_ref, at_ref, ab_ref, bt_ref, bb_ref)):
        project(ref[...], gain, cols, rows, out_ref, place * ref.shape[0])


def far_kernel(near_ref, ot_ref, ob_ref, gain_ref, cols_ref, rows_ref, full_ref, head_ref, tail_ref):
    chunk = near_ref.shape[0] // 3
    half = chunk // 2
    total = full_ref.shape[0]
    place = lax.axis_index("tp")
    for slot, shift in enumerate((0, 3, 1)):
        start = pl.multiple_of(lax.rem(place + shift, 4) * chunk, 64)
        full_ref[pl.ds(start, chunk), :] = near_ref[slot * chunk : (slot + 1) * chunk, :]
    gain, cols, rows = gain_ref[...], cols_ref[...], rows_ref[...]
    for part, ref in enumerate((ot_ref, ob_ref)):
        start = pl.multiple_of(lax.rem(place + 2, 4) * chunk + part * half, 32)
        project(ref[...], gain, cols, rows, full_ref, start)
    lane = lax.broadcasted_iota(jnp.int32, (WIN, LANES), 1)
    for ref, rows, edge in ((head_ref, 0, 0), (tail_ref, total - WIN, total - EDGE)):
        keys = full_ref[rows : rows + WIN, 3 * LANES : 4 * LANES].astype(F32)
        values = full_ref[rows : rows + WIN, 4 * LANES :].astype(F32)
        ref[:WIN, :] = jnp.where(lane < HEAD, keys, values).astype(BF16)
        ref[WIN:, :] = full_ref[edge : edge + EDGE, 2 * LANES : 3 * LANES]


def mix_kernel(sink_ref, taps_ref, full_ref, low_ref, high_ref, out_ref, key_ref, value_ref, conv_ref, *, last):
    total = full_ref.shape[0]
    lane = lax.broadcasted_iota(jnp.int32, (WIN, LANES), 1)
    for ref, row in ((low_ref, 0), (high_ref, WIN + total)):
        pair = ref[:WIN, :].astype(F32)
        turned = pltpu.roll(pair, HEAD, 1)
        key_ref[row : row + WIN, :] = jnp.where(lane < HEAD, pair, turned).astype(BF16)
        value_ref[row : row + WIN, :] = jnp.where(lane < HEAD, turned, pair).astype(BF16)
    key_ref[WIN : WIN + total, :] = full_ref[:, 3 * LANES : 4 * LANES]
    value_ref[WIN : WIN + total, :] = full_ref[:, 4 * LANES :]

    conv_ref[0:8, :] = low_ref[WIN + EDGE - 8 :, :].astype(F32)
    conv_ref[8 : 8 + total, :] = full_ref[:, 2 * LANES : 3 * LANES].astype(F32)
    conv_ref[8 + total :, :] = high_ref[WIN : WIN + 8, :].astype(F32)
    convolved = (
        taps_ref[0:1, :] * conv_ref[7 : 7 + total, :]
        + taps_ref[1:2, :] * conv_ref[8 : 8 + total, :]
        + taps_ref[2:3, :] * conv_ref[9 : 9 + total, :]
    )
    gate = full_ref[:, LANES : 2 * LANES].astype(F32)
    out_ref[:, LANES:] = (gate * convolved).astype(BF16)

    place = lax.axis_index("sp")
    row = lax.broadcasted_iota(jnp.int32, (2 * WIN, 3 * WIN), 0)
    col = lax.broadcasted_iota(jnp.int32, (2 * WIN, 3 * WIN), 1)
    rel = col - lax.rem(row, WIN)
    band = (rel >= 0) & (rel <= 2 * WIN)
    half = lax.broadcasted_iota(jnp.int32, (2 * WIN, 1), 0) < WIN
    sink = jnp.where(half, sink_ref[0], sink_ref[1])
    blocks = total // WIN
    for block in range(blocks):
        at = block * WIN
        query = full_ref[at : at + WIN, :LANES]
        zero = jnp.zeros_like(query)
        both = jnp.concatenate([jnp.where(lane < HEAD, query, zero), jnp.where(lane < HEAD, zero, query)], axis=0)
        score = lax.dot_general(
            both, key_ref[at : at + 3 * WIN, :], (((1,), (1,)), ((), ())), preferred_element_type=F32
        ) * HEAD ** (-0.5)
        allowed = band
        if block == 0:
            allowed = allowed & (col >= jnp.where(place == 0, WIN, 0))
        if block == blocks - 1:
            allowed = allowed & (col < jnp.where(place == last, 2 * WIN, 3 * WIN))
        score = jnp.where(allowed, score, -jnp.inf)
        top = jnp.maximum(jnp.max(score, axis=-1, keepdims=True), sink)
        expo = jnp.exp(score - top)
        denom = jnp.sum(expo, axis=-1, keepdims=True) + jnp.exp(sink - top)
        weights = (expo * (1.0 / denom)).astype(BF16)
        got = jnp.dot(weights, value_ref[at : at + 3 * WIN, :], preferred_element_type=F32)
        out_ref[at : at + WIN, :LANES] = jnp.where(lane < HEAD, got[:WIN], got[WIN:]).astype(BF16)


def out_kernel(parts_ref, weight_ref, out_ref):
    count = parts_ref.shape[0]
    joined = jnp.concatenate(
        [parts_ref[i, :, :LANES] for i in range(count)] + [parts_ref[i, :, LANES:] for i in range(count)], axis=1
    )
    out_ref[...] = jnp.dot(joined, weight_ref[...], preferred_element_type=F32).astype(BF16)


def body(
    tokens,
    norm_gain,
    query_weight,
    key_weight,
    value_weight,
    sink_logit,
    conv_gate_weight,
    conv_pre_weight,
    conv_input_weight,
    conv_taps,
    out_weight,
):
    chunk, width = tokens.shape
    total = 4 * chunk
    half = chunk // 2
    forward = [(i, (i + 1) % 4) for i in range(4)]
    backward = [(i, (i + 3) % 4) for i in range(4)]
    top, bottom = pl.pallas_call(
        split_kernel,
        name="split",
        out_shape=(pltpu.VMEM((half, width), BF16), pltpu.VMEM((half, width), BF16)),
        in_specs=[pl.BlockSpec(memory_space=pltpu.HBM)],
        out_specs=(VMEM, VMEM),
        scratch_shapes=[pltpu.SemaphoreType.DMA((2,))],
        compiler_params=params(16),
    )(pltpu.with_memory_space_constraint(tokens, pltpu.HBM))
    before_top = lax.ppermute(top, "tp", forward)
    after_bottom = lax.ppermute(bottom, "tp", backward)
    before_bottom = lax.ppermute(bottom, "tp", forward)
    after_top = lax.ppermute(top, "tp", backward)
    far_top = lax.ppermute(before_top, "tp", forward)
    far_bottom = lax.ppermute(after_bottom, "tp", backward)

    cols, rows = pl.pallas_call(
        pack_kernel,
        name="pack",
        out_shape=(pltpu.VMEM((width, 4 * LANES), BF16), pltpu.VMEM((2 * LANES, width), BF16)),
        in_specs=[VMEM] * 6,
        out_specs=(VMEM, VMEM),
        compiler_params=params(16),
    )(query_weight, key_weight.T, value_weight.T, conv_gate_weight, conv_pre_weight, conv_input_weight)
    gain = norm_gain.reshape(1, width)
    near = pl.pallas_call(
        near_kernel,
        name="near",
        out_shape=pltpu.VMEM((3 * chunk, 5 * LANES), BF16),
        in_specs=[VMEM] * 9,
        out_specs=VMEM,
        compiler_params=params(16),
    )(*near_memory(top, bottom, before_top, before_bottom, after_top, after_bottom, gain, cols, rows))
    full, head, tail = pl.pallas_call(
        far_kernel,
        name="far",
        out_shape=(
            pltpu.VMEM((total, 5 * LANES), BF16),
            pltpu.VMEM((WIN + EDGE, LANES), BF16),
            pltpu.VMEM((WIN + EDGE, LANES), BF16),
        ),
        in_specs=[VMEM] * 6,
        out_specs=(VMEM, VMEM, VMEM),
        compiler_params=params(16),
    )(*near_memory(near, far_top, far_bottom, gain, cols, rows))

    count = lax.axis_size("sp")
    up = [(i, i + 1) for i in range(count - 1)]
    down = [(i + 1, i) for i in range(count - 1)]
    low = lax.ppermute(tail, "sp", up)
    high = lax.ppermute(head, "sp", down)

    def mix(*refs):
        mix_kernel(*refs, last=count - 1)

    mixed = pl.pallas_call(
        mix,
        name="mix",
        out_shape=pltpu.VMEM((total, 2 * LANES), BF16),
        in_specs=[SMEM] + [VMEM] * 4,
        compiler_params=params(16),
        out_specs=VMEM,
        scratch_shapes=[
            pltpu.VMEM((total + 2 * WIN, LANES), BF16),
            pltpu.VMEM((total + 2 * WIN, LANES), BF16),
            pltpu.VMEM((total + 16, LANES), F32),
        ],
    )(sink_logit, *near_memory(conv_taps, full, low, high))
    parts = lax.all_to_all(mixed.reshape(4, chunk, 2 * LANES), "tp", split_axis=0, concat_axis=0, tiled=True)
    step = 512
    parts, out_weight = near_memory(parts, out_weight)
    return pl.pallas_call(
        out_kernel,
        name="project_out",
        out_shape=jax.ShapeDtypeStruct((chunk, out_weight.shape[1]), BF16),
        grid=(out_weight.shape[1] // step,),
        in_specs=[
            pl.BlockSpec((4, chunk, 2 * LANES), lambda i: (0, 0, 0)),
            pl.BlockSpec((out_weight.shape[0], step), lambda i: (0, i)),
        ],
        out_specs=pl.BlockSpec((chunk, step), lambda i: (0, i)),
        compiler_params=params(16),
    )(parts, out_weight)


def solution(mesh):
    placed = (
        P(("sp", "tp"), None),
        P(),
        P(None, "tp"),
        P(None, "tp"),
        P(None, "tp"),
        P("tp"),
        P(None, "tp"),
        P(None, "tp"),
        P(None, "tp"),
        P(None, "tp"),
        P(),
    )
    return jax.shard_map(
        body, mesh=mesh, in_specs=placed, out_specs=P(("sp", "tp"), None), check_vma=False
    )
```

```python
import jax
import jax.numpy as jnp
from jax import lax
from jax.experimental import pallas as pl
from jax.experimental.pallas import tpu as pltpu
from jax.sharding import PartitionSpec as P


HEAD = 64
WIN = 128
EDGE = 16
LANES = 128
F32 = jnp.float32
BF16 = jnp.bfloat16
VMEM = pl.BlockSpec(memory_space=pltpu.VMEM)
SMEM = pl.BlockSpec(memory_space=pltpu.SMEM)


def near_memory(*arrays):
    return tuple(pltpu.with_memory_space_constraint(array, pltpu.VMEM) for array in arrays)


def params(mebibytes):
    return pltpu.CompilerParams(vmem_limit_bytes=mebibytes << 20)


def run_copies(pairs, sems):
    copies = [pltpu.make_async_copy(source, target, sems.at[i]) for i, (source, target) in enumerate(pairs)]
    for copy in copies:
        copy.start()
    for copy in copies:
        copy.wait()


def split_kernel(tokens_ref, top_ref, bottom_ref, sems):
    rows = top_ref.shape[0]
    run_copies(
        (
            (tokens_ref.at[pl.ds(0, rows)], top_ref),
            (tokens_ref.at[pl.ds(rows, bottom_ref.shape[0])], bottom_ref),
        ),
        sems,
    )


def pack_kernel(q_ref, k_ref, v_ref, gate_ref, pre_ref, input_ref, gain_ref, cols_ref, rows_ref, gain_out_ref, sems):
    pairs = [
        (ref, cols_ref.at[:, pl.ds(place * LANES, LANES)])
        for place, ref in enumerate((q_ref, gate_ref, pre_ref, input_ref))
    ]
    pairs += [
        (ref, rows_ref.at[pl.ds(place * HEAD, HEAD)]) for place, ref in enumerate((k_ref, k_ref, v_ref, v_ref))
    ]
    run_copies(pairs + [(gain_ref, gain_out_ref)], sems)


def project(rows, gain, cols, kv_rows, out_ref, start):
    count = rows.shape[0]
    rows = rows.astype(F32)
    scale = lax.rsqrt(jnp.mean(rows * rows, axis=-1, keepdims=True) + 1e-06)
    normed = (rows * scale * gain).astype(BF16)
    out = jnp.dot(normed, cols, preferred_element_type=F32).astype(BF16)
    product = out[:, 2 * LANES : 3 * LANES].astype(F32) * out[:, 3 * LANES :].astype(F32)
    pairs = lax.dot_general(normed, kv_rows, (((1,), (1,)), ((), ())), preferred_element_type=F32)
    out_ref[pl.ds(start, count), : 2 * LANES] = out[:, : 2 * LANES]
    out_ref[pl.ds(start, count), 2 * LANES : 3 * LANES] = product.astype(BF16)
    out_ref[pl.ds(start, count), 3 * LANES :] = pairs.astype(BF16)


def take_edge(full_ref, edge_ref, tail):
    total = full_ref.shape[0]
    pair = pl.multiple_of(jnp.where(tail, total - WIN, 0), EDGE)
    lane = lax.broadcasted_iota(jnp.int32, (WIN, LANES), 1)
    keys = full_ref[pl.ds(pair, WIN), 3 * LANES : 4 * LANES].astype(F32)
    values = full_ref[pl.ds(pair, WIN), 4 * LANES :].astype(F32)
    edge_ref[:WIN, :] = jnp.where(lane < HEAD, keys, values).astype(BF16)
    edge = pl.multiple_of(jnp.where(tail, total - EDGE, 0), EDGE)
    edge_ref[WIN:, :] = full_ref[pl.ds(edge, EDGE), 2 * LANES : 3 * LANES]


def near_kernel(*refs):
    *pieces, gain_ref, cols_ref, rows_ref, full_ref, early_ref = refs
    gain, cols, rows = gain_ref[...], cols_ref[...], rows_ref[...]
    place = lax.axis_index("tp")
    chunk = full_ref.shape[0] // 4
    for slot, turn in enumerate((0, 3, 1)):
        start = lax.rem(place + turn, 4) * chunk
        for ref in pieces[2 * slot : 2 * slot + 2]:
            project(ref[...], gain, cols, rows, full_ref, pl.multiple_of(start, EDGE))
            start = start + ref.shape[0]
    take_edge(full_ref, early_ref, place != 1)


def far_kernel(near_ref, top_ref, bottom_ref, gain_ref, cols_ref, rows_ref, full_ref, late_ref):
    gain, cols, rows = gain_ref[...], cols_ref[...], rows_ref[...]
    place = lax.axis_index("tp")
    start = lax.rem(place + 2, 4) * (full_ref.shape[0] // 4)
    for ref in (top_ref, bottom_ref):
        project(ref[...], gain, cols, rows, full_ref, pl.multiple_of(start, EDGE))
        start = start + ref.shape[0]
    take_edge(full_ref, late_ref, place == 1)


def attend(query, keys, values, sink, lowest, highest):
    lane = lax.broadcasted_iota(jnp.int32, (WIN, LANES), 1)
    row = lax.broadcasted_iota(jnp.int32, (2 * WIN, 3 * WIN), 0)
    col = lax.broadcasted_iota(jnp.int32, (2 * WIN, 3 * WIN), 1)
    rel = col - lax.rem(row, WIN)
    allowed = (rel >= 0) & (rel <= 2 * WIN)
    if lowest is not None:
        allowed = allowed & (col >= lowest)
    if highest is not None:
        allowed = allowed & (col < highest)
    zero = jnp.zeros_like(query)
    both = jnp.concatenate([jnp.where(lane < HEAD, query, zero), jnp.where(lane < HEAD, zero, query)], axis=0)
    score = lax.dot_general(both, keys, (((1,), (1,)), ((), ())), preferred_element_type=F32) * HEAD ** (-0.5)
    score = jnp.where(allowed, score, -jnp.inf)
    top = jnp.maximum(jnp.max(score, axis=-1, keepdims=True), sink)
    expo = jnp.exp(score - top)
    denom = jnp.sum(expo, axis=-1, keepdims=True) + jnp.exp(sink - top)
    weights = (expo * (1.0 / denom)).astype(BF16)
    got = jnp.dot(weights, values, preferred_element_type=F32)
    return jnp.where(lane < HEAD, got[:WIN], got[WIN:]).astype(BF16)


def sink_column(sink_ref):
    half = lax.broadcasted_iota(jnp.int32, (2 * WIN, 1), 0) < WIN
    return jnp.where(half, sink_ref[0], sink_ref[1])


def convolve(taps_ref, conv_ref, count):
    return (
        taps_ref[0:1, :] * conv_ref[7 : 7 + count, :]
        + taps_ref[1:2, :] * conv_ref[8 : 8 + count, :]
        + taps_ref[2:3, :] * conv_ref[9 : 9 + count, :]
    )


def inner_kernel(sink_ref, taps_ref, full_ref, out_ref, conv_ref):
    total = full_ref.shape[0]
    conv_ref[0:8, :] = jnp.zeros((8, LANES), F32)
    conv_ref[8 : 8 + total, :] = full_ref[:, 2 * LANES : 3 * LANES].astype(F32)
    conv_ref[8 + total :, :] = jnp.zeros((8, LANES), F32)
    gate = full_ref[:, LANES : 2 * LANES].astype(F32)
    out_ref[:, LANES:] = (gate * convolve(taps_ref, conv_ref, total)).astype(BF16)
    sink = sink_column(sink_ref)
    for at in range(WIN, total - WIN, WIN):
        window = slice(at - WIN, at + 2 * WIN)
        out_ref[at : at + WIN, :LANES] = attend(
            full_ref[at : at + WIN, :LANES],
            full_ref[window, 3 * LANES : 4 * LANES],
            full_ref[window, 4 * LANES :],
            sink,
            None,
            None,
        )


def outer_kernel(sink_ref, taps_ref, full_ref, inner_ref, early_ref, late_ref, out_ref, conv_ref, *, last):
    total = full_ref.shape[0]
    place = lax.axis_index("sp")
    swapped = lax.axis_index("tp") == 1
    early, late = early_ref[...].astype(F32), late_ref[...].astype(F32)
    low, high = jnp.where(swapped, late, early), jnp.where(swapped, early, late)
    lane = lax.broadcasted_iota(jnp.int32, (WIN, LANES), 1)

    def unpack(halo):
        pair = halo[:WIN]
        turned = pltpu.roll(pair, HEAD, 1)
        keys, values = jnp.where(lane < HEAD, pair, turned), jnp.where(lane < HEAD, turned, pair)
        return keys.astype(BF16), values.astype(BF16)

    sink = sink_column(sink_ref)
    for at, halo in ((0, low), (total - WIN, high)):
        first = at == 0
        window = slice(0, 2 * WIN) if first else slice(total - 2 * WIN, total)
        sides = []
        for piece, lanes in zip(unpack(halo), (3, 4)):
            own = full_ref[window, lanes * LANES : (lanes + 1) * LANES]
            sides.append(jnp.concatenate([piece, own] if first else [own, piece], axis=0))
        out_ref[at : at + WIN, :LANES] = attend(
            full_ref[at : at + WIN, :LANES],
            *sides,
            sink,
            jnp.where(place == 0, WIN, 0) if first else None,
            None if first else jnp.where(place == last, 2 * WIN, 3 * WIN),
        )
        if first:
            conv_ref[0:8, :] = halo[WIN + EDGE - 8 :]
            conv_ref[8:32, :] = full_ref[0:32, 2 * LANES : 3 * LANES].astype(F32)[:24]
        else:
            conv_ref[0:24, :] = full_ref[total - 32 :, 2 * LANES : 3 * LANES].astype(F32)[8:]
            conv_ref[24:32, :] = halo[WIN : WIN + 8]
        rows = slice(0, EDGE) if first else slice(total - EDGE, total)
        gate = full_ref[rows, LANES : 2 * LANES].astype(F32)
        out_ref[rows, LANES:] = (gate * convolve(taps_ref, conv_ref, EDGE)).astype(BF16)


def out_kernel(parts_ref, weight_ref, out_ref, done_ref, sems):
    count = parts_ref.shape[0]
    joined = jnp.concatenate(
        [parts_ref[i, :, :LANES] for i in range(count)] + [parts_ref[i, :, LANES:] for i in range(count)], axis=1
    )
    steps, _, step = done_ref.shape
    copies = []
    for i in range(steps):
        columns = pl.ds(i * step, step)
        done_ref[i] = jnp.dot(joined, weight_ref[:, columns], preferred_element_type=F32).astype(BF16)
        copies.append(pltpu.make_async_copy(done_ref.at[i], out_ref.at[:, columns], sems.at[i]))
        copies[-1].start()
    for copy in copies:
        copy.wait()


def body(
    tokens,
    norm_gain,
    query_weight,
    key_weight,
    value_weight,
    sink_logit,
    conv_gate_weight,
    conv_pre_weight,
    conv_input_weight,
    conv_taps,
    out_weight,
):
    chunk, width = tokens.shape
    total = 4 * chunk

    def local(kernel, shapes, count, **more):
        return pl.pallas_call(
            kernel,
            out_shape=tuple(pltpu.VMEM(shape, dtype) for shape, dtype in shapes),
            in_specs=[VMEM] * count,
            out_specs=(VMEM,) * len(shapes),
            compiler_params=params(16),
            **more,
        )

    def in_hbm(*arrays):
        return tuple(pltpu.with_memory_space_constraint(array, pltpu.HBM) for array in arrays)

    def loader(kernel, shapes, count):
        return pl.pallas_call(
            kernel,
            out_shape=tuple(pltpu.VMEM(shape, dtype) for shape, dtype in shapes),
            in_specs=[pl.BlockSpec(memory_space=pltpu.HBM)] * count,
            out_specs=(VMEM,) * len(shapes),
            scratch_shapes=[pltpu.SemaphoreType.DMA((9,))],
            compiler_params=params(16),
        )

    forward = [(i, (i + 1) % 4) for i in range(4)]
    backward = [(i, (i + 3) % 4) for i in range(4)]
    lead = chunk // 2 + EDGE
    top, bottom = loader(split_kernel, (((lead, width), BF16), ((chunk - lead, width), BF16)), 1)(*in_hbm(tokens))

    before_top = lax.ppermute(top, "tp", forward)
    after_bottom = lax.ppermute(bottom, "tp", backward)
    before_bottom = lax.ppermute(bottom, "tp", forward)
    after_top = lax.ppermute(top, "tp", backward)
    far_top = lax.ppermute(before_top, "tp", forward)
    far_bottom = lax.ppermute(after_bottom, "tp", backward)

    packed = loader(pack_kernel, (((width, 4 * LANES), BF16), ((2 * LANES, width), BF16), ((1, width), F32)), 7)(
        *in_hbm(
            query_weight,
            key_weight.T,
            value_weight.T,
            conv_gate_weight,
            conv_pre_weight,
            conv_input_weight,
            norm_gain.reshape(1, width),
        )
    )
    cols, rows, gain = packed
    weights = (gain, cols, rows)
    full_shape = ((total, 5 * LANES), BF16)
    edge_shape = ((WIN + EDGE, LANES), BF16)
    full, early = local(near_kernel, (full_shape, edge_shape), 9)(
        *near_memory(top, bottom, before_top, before_bottom, after_top, after_bottom, *weights)
    )
    count = lax.axis_size("sp")
    ups = {x: [(4 * i + x, 4 * i + 4 + x) for i in range(count - 1)] for x in range(4)}
    downs = {x: [(j, i) for i, j in pairs] for x, pairs in ups.items()}
    early = lax.ppermute(early, ("sp", "tp"), ups[0] + downs[1] + ups[2] + ups[3])
    full, late = local(far_kernel, (full_shape, edge_shape), 6, input_output_aliases={0: 0})(
        *near_memory(full, far_top, far_bottom, *weights)
    )
    late = lax.ppermute(late, ("sp", "tp"), downs[0] + ups[1] + downs[2] + downs[3])

    def outer(*refs):
        outer_kernel(*refs, last=count - 1)

    def mixer(kernel, inputs, rows, **more):
        return pl.pallas_call(
            kernel,
            out_shape=pltpu.VMEM((total, 2 * LANES), BF16),
            in_specs=[SMEM] + [VMEM] * inputs,
            out_specs=VMEM,
            scratch_shapes=[pltpu.VMEM((rows, LANES), F32)],
            compiler_params=params(16),
            **more,
        )

    (taps,) = near_memory(conv_taps)
    inner = mixer(inner_kernel, 2, total + 16)(sink_logit, taps, *near_memory(full))
    mixed = mixer(outer, 5, 32, input_output_aliases={3: 0})(sink_logit, taps, *near_memory(full, inner, early, late))
    parts = lax.all_to_all(mixed.reshape(4, chunk, 2 * LANES), "tp", split_axis=0, concat_axis=0, tiled=True)
    step = 512
    steps = out_weight.shape[1] // step
    return pl.pallas_call(
        out_kernel,
        name="project_out",
        out_shape=jax.ShapeDtypeStruct((chunk, out_weight.shape[1]), BF16),
        in_specs=[VMEM] * 2,
        out_specs=pl.BlockSpec(memory_space=pltpu.HBM),
        scratch_shapes=[pltpu.VMEM((steps, chunk, step), BF16), pltpu.SemaphoreType.DMA((steps,))],
        compiler_params=params(16),
    )(*near_memory(parts, out_weight))


def solution(mesh):
    placed = (
        P(("sp", "tp"), None),
        P(),
        P(None, "tp"),
        P(None, "tp"),
        P(None, "tp"),
        P("tp"),
        P(None, "tp"),
        P(None, "tp"),
        P(None, "tp"),
        P(None, "tp"),
        P(),
    )

    return jax.shard_map(body, mesh=mesh, in_specs=placed, out_specs=P(("sp", "tp"), None), check_vma=False)
```

```python
import jax
import jax.numpy as jnp
from jax import lax
from jax.experimental import pallas as pl
from jax.experimental.pallas import tpu as pltpu
from jax.sharding import PartitionSpec as P


HEAD = 64
WIN = 128
EDGE = 16
LANES = 128
F32 = jnp.float32
BF16 = jnp.bfloat16
VMEM = pl.BlockSpec(memory_space=pltpu.VMEM)
SMEM = pl.BlockSpec(memory_space=pltpu.SMEM)


def near_memory(*arrays):
    return tuple(pltpu.with_memory_space_constraint(array, pltpu.VMEM) for array in arrays)


def params(mebibytes):
    return pltpu.CompilerParams(vmem_limit_bytes=mebibytes << 20)


def run_copies(pairs, sems):
    copies = [pltpu.make_async_copy(source, target, sems.at[i]) for i, (source, target) in enumerate(pairs)]
    for copy in copies:
        copy.start()
    for copy in copies:
        copy.wait()


def split_kernel(tokens_ref, top_ref, bottom_ref, sems):
    rows = top_ref.shape[0]
    run_copies(
        (
            (tokens_ref.at[pl.ds(0, rows)], top_ref),
            (tokens_ref.at[pl.ds(rows, bottom_ref.shape[0])], bottom_ref),
        ),
        sems,
    )


def pack_kernel(q_ref, k_ref, v_ref, gate_ref, pre_ref, input_ref, gain_ref, cols_ref, rows_ref, gain_out_ref, sems):
    pairs = [
        (ref, cols_ref.at[:, pl.ds(place * LANES, LANES)])
        for place, ref in enumerate((q_ref, gate_ref, pre_ref, input_ref))
    ]
    pairs += [
        (ref, rows_ref.at[pl.ds(place * HEAD, HEAD)]) for place, ref in enumerate((k_ref, k_ref, v_ref, v_ref))
    ]
    run_copies(pairs + [(gain_ref, gain_out_ref)], sems)


def project(rows, gain, cols, kv_rows, out_ref, start):
    count = rows.shape[0]
    rows = rows.astype(F32)
    scale = lax.rsqrt(jnp.mean(rows * rows, axis=-1, keepdims=True) + 1e-06)
    normed = (rows * scale * gain).astype(BF16)
    out = jnp.dot(normed, cols, preferred_element_type=F32).astype(BF16)
    product = out[:, 2 * LANES : 3 * LANES].astype(F32) * out[:, 3 * LANES :].astype(F32)
    pairs = lax.dot_general(normed, kv_rows, (((1,), (1,)), ((), ())), preferred_element_type=F32)
    out_ref[pl.ds(start, count), : 2 * LANES] = out[:, : 2 * LANES]
    out_ref[pl.ds(start, count), 2 * LANES : 3 * LANES] = product.astype(BF16)
    out_ref[pl.ds(start, count), 3 * LANES :] = pairs.astype(BF16)


def take_edge(full_ref, edge_ref, tail):
    total = full_ref.shape[0]
    pair = pl.multiple_of(jnp.where(tail, total - WIN, 0), EDGE)
    lane = lax.broadcasted_iota(jnp.int32, (WIN, LANES), 1)
    keys = full_ref[pl.ds(pair, WIN), 3 * LANES : 4 * LANES].astype(F32)
    values = full_ref[pl.ds(pair, WIN), 4 * LANES :].astype(F32)
    edge_ref[:WIN, :] = jnp.where(lane < HEAD, keys, values).astype(BF16)
    edge = pl.multiple_of(jnp.where(tail, total - EDGE, 0), EDGE)
    edge_ref[WIN:, :] = full_ref[pl.ds(edge, EDGE), 2 * LANES : 3 * LANES]


def near_kernel(*refs):
    *pieces, gain_ref, cols_ref, rows_ref, full_ref, early_ref = refs
    gain, cols, rows = gain_ref[...], cols_ref[...], rows_ref[...]
    place = lax.axis_index("tp")
    chunk = full_ref.shape[0] // 4
    for slot, turn in enumerate((0, 1, 3)):
        start = (place ^ turn) * chunk
        for ref in pieces[2 * slot : 2 * slot + 2]:
            project(ref[...], gain, cols, rows, full_ref, pl.multiple_of(start, EDGE))
            start = start + ref.shape[0]
    take_edge(full_ref, early_ref, place != 1)


def far_kernel(near_ref, top_ref, bottom_ref, gain_ref, cols_ref, rows_ref, full_ref, late_ref):
    gain, cols, rows = gain_ref[...], cols_ref[...], rows_ref[...]
    place = lax.axis_index("tp")
    start = (place ^ 2) * (full_ref.shape[0] // 4)
    for ref in (top_ref, bottom_ref):
        project(ref[...], gain, cols, rows, full_ref, pl.multiple_of(start, EDGE))
        start = start + ref.shape[0]
    take_edge(full_ref, late_ref, place == 1)


def attend(query, keys, values, sink, lowest, highest):
    lane = lax.broadcasted_iota(jnp.int32, (WIN, LANES), 1)
    row = lax.broadcasted_iota(jnp.int32, (2 * WIN, 3 * WIN), 0)
    col = lax.broadcasted_iota(jnp.int32, (2 * WIN, 3 * WIN), 1)
    rel = col - lax.rem(row, WIN)
    allowed = (rel >= 0) & (rel <= 2 * WIN)
    if lowest is not None:
        allowed = allowed & (col >= lowest)
    if highest is not None:
        allowed = allowed & (col < highest)
    zero = jnp.zeros_like(query)
    both = jnp.concatenate([jnp.where(lane < HEAD, query, zero), jnp.where(lane < HEAD, zero, query)], axis=0)
    score = lax.dot_general(both, keys, (((1,), (1,)), ((), ())), preferred_element_type=F32) * HEAD ** (-0.5)
    score = jnp.where(allowed, score, -jnp.inf)
    top = jnp.maximum(jnp.max(score, axis=-1, keepdims=True), sink)
    expo = jnp.exp(score - top)
    denom = jnp.sum(expo, axis=-1, keepdims=True) + jnp.exp(sink - top)
    weights = (expo * (1.0 / denom)).astype(BF16)
    got = jnp.dot(weights, values, preferred_element_type=F32)
    return jnp.where(lane < HEAD, got[:WIN], got[WIN:]).astype(BF16)


def sink_column(sink_ref):
    half = lax.broadcasted_iota(jnp.int32, (2 * WIN, 1), 0) < WIN
    return jnp.where(half, sink_ref[0], sink_ref[1])


def convolve(taps_ref, conv_ref, count):
    return (
        taps_ref[0:1, :] * conv_ref[7 : 7 + count, :]
        + taps_ref[1:2, :] * conv_ref[8 : 8 + count, :]
        + taps_ref[2:3, :] * conv_ref[9 : 9 + count, :]
    )


def inner_kernel(sink_ref, taps_ref, full_ref, out_ref, conv_ref):
    total = full_ref.shape[0]
    conv_ref[0:8, :] = jnp.zeros((8, LANES), F32)
    conv_ref[8 : 8 + total, :] = full_ref[:, 2 * LANES : 3 * LANES].astype(F32)
    conv_ref[8 + total :, :] = jnp.zeros((8, LANES), F32)
    gate = full_ref[:, LANES : 2 * LANES].astype(F32)
    out_ref[:, LANES:] = (gate * convolve(taps_ref, conv_ref, total)).astype(BF16)
    sink = sink_column(sink_ref)
    for at in range(WIN, total - WIN, WIN):
        window = slice(at - WIN, at + 2 * WIN)
        out_ref[at : at + WIN, :LANES] = attend(
            full_ref[at : at + WIN, :LANES],
            full_ref[window, 3 * LANES : 4 * LANES],
            full_ref[window, 4 * LANES :],
            sink,
            None,
            None,
        )


def outer_kernel(sink_ref, taps_ref, full_ref, inner_ref, early_ref, late_ref, out_ref, conv_ref, *, last):
    total = full_ref.shape[0]
    place = lax.axis_index("sp")
    swapped = lax.axis_index("tp") == 1
    early, late = early_ref[...].astype(F32), late_ref[...].astype(F32)
    low, high = jnp.where(swapped, late, early), jnp.where(swapped, early, late)
    lane = lax.broadcasted_iota(jnp.int32, (WIN, LANES), 1)

    def unpack(halo):
        pair = halo[:WIN]
        turned = pltpu.roll(pair, HEAD, 1)
        keys, values = jnp.where(lane < HEAD, pair, turned), jnp.where(lane < HEAD, turned, pair)
        return keys.astype(BF16), values.astype(BF16)

    sink = sink_column(sink_ref)
    for at, halo in ((0, low), (total - WIN, high)):
        first = at == 0
        window = slice(0, 2 * WIN) if first else slice(total - 2 * WIN, total)
        sides = []
        for piece, lanes in zip(unpack(halo), (3, 4)):
            own = full_ref[window, lanes * LANES : (lanes + 1) * LANES]
            sides.append(jnp.concatenate([piece, own] if first else [own, piece], axis=0))
        out_ref[at : at + WIN, :LANES] = attend(
            full_ref[at : at + WIN, :LANES],
            *sides,
            sink,
            jnp.where(place == 0, WIN, 0) if first else None,
            None if first else jnp.where(place == last, 2 * WIN, 3 * WIN),
        )
        if first:
            conv_ref[0:8, :] = halo[WIN + EDGE - 8 :]
            conv_ref[8:32, :] = full_ref[0:32, 2 * LANES : 3 * LANES].astype(F32)[:24]
        else:
            conv_ref[0:24, :] = full_ref[total - 32 :, 2 * LANES : 3 * LANES].astype(F32)[8:]
            conv_ref[24:32, :] = halo[WIN : WIN + 8]
        rows = slice(0, EDGE) if first else slice(total - EDGE, total)
        gate = full_ref[rows, LANES : 2 * LANES].astype(F32)
        out_ref[rows, LANES:] = (gate * convolve(taps_ref, conv_ref, EDGE)).astype(BF16)


def out_kernel(parts_ref, weight_ref, out_ref, done_ref, sems):
    count = parts_ref.shape[0]
    joined = jnp.concatenate(
        [parts_ref[i, :, :LANES] for i in range(count)] + [parts_ref[i, :, LANES:] for i in range(count)], axis=1
    )
    steps, _, step = done_ref.shape
    copies = []
    for i in range(steps):
        columns = pl.ds(i * step, step)
        done_ref[i] = jnp.dot(joined, weight_ref[:, columns], preferred_element_type=F32).astype(BF16)
        copies.append(pltpu.make_async_copy(done_ref.at[i], out_ref.at[:, columns], sems.at[i]))
        copies[-1].start()
    for copy in copies:
        copy.wait()


def body(
    tokens,
    norm_gain,
    query_weight,
    key_weight,
    value_weight,
    sink_logit,
    conv_gate_weight,
    conv_pre_weight,
    conv_input_weight,
    conv_taps,
    out_weight,
):
    chunk, width = tokens.shape
    total = 4 * chunk

    def local(kernel, shapes, count, **more):
        return pl.pallas_call(
            kernel,
            out_shape=tuple(pltpu.VMEM(shape, dtype) for shape, dtype in shapes),
            in_specs=[VMEM] * count,
            out_specs=(VMEM,) * len(shapes),
            compiler_params=params(16),
            **more,
        )

    def in_hbm(*arrays):
        return tuple(pltpu.with_memory_space_constraint(array, pltpu.HBM) for array in arrays)

    def loader(kernel, shapes, count):
        return pl.pallas_call(
            kernel,
            out_shape=tuple(pltpu.VMEM(shape, dtype) for shape, dtype in shapes),
            in_specs=[pl.BlockSpec(memory_space=pltpu.HBM)] * count,
            out_specs=(VMEM,) * len(shapes),
            scratch_shapes=[pltpu.SemaphoreType.DMA((9,))],
            compiler_params=params(16),
        )

    lead = chunk // 2 - EDGE
    top, bottom = loader(split_kernel, (((lead, width), BF16), ((chunk - lead, width), BF16)), 1)(*in_hbm(tokens))

    def swap(block, turn):
        return lax.ppermute(block, "tp", [(i, i ^ turn) for i in range(4)])

    a_top = swap(top, 1)
    b_bottom = swap(bottom, 3)
    a_bottom = swap(bottom, 1)
    b_top = swap(top, 3)
    far_top = swap(a_top, 3)
    far_bottom = swap(b_bottom, 1)

    packed = loader(pack_kernel, (((width, 4 * LANES), BF16), ((2 * LANES, width), BF16), ((1, width), F32)), 7)(
        *in_hbm(
            query_weight,
            key_weight.T,
            value_weight.T,
            conv_gate_weight,
            conv_pre_weight,
            conv_input_weight,
            norm_gain.reshape(1, width),
        )
    )
    cols, rows, gain = packed
    weights = (gain, cols, rows)
    full_shape = ((total, 5 * LANES), BF16)
    edge_shape = ((WIN + EDGE, LANES), BF16)
    full, early = local(near_kernel, (full_shape, edge_shape), 9)(
        *near_memory(top, bottom, a_top, a_bottom, b_top, b_bottom, *weights)
    )
    count = lax.axis_size("sp")
    ups = {x: [(4 * i + x, 4 * i + 4 + x) for i in range(count - 1)] for x in range(4)}
    downs = {x: [(j, i) for i, j in pairs] for x, pairs in ups.items()}
    early = lax.ppermute(early, ("sp", "tp"), ups[0] + downs[1] + ups[2] + ups[3])
    full, late = local(far_kernel, (full_shape, edge_shape), 6, input_output_aliases={0: 0})(
        *near_memory(full, far_top, far_bottom, *weights)
    )
    late = lax.ppermute(late, ("sp", "tp"), downs[0] + ups[1] + downs[2] + downs[3])

    def outer(*refs):
        outer_kernel(*refs, last=count - 1)

    def mixer(kernel, inputs, rows, **more):
        return pl.pallas_call(
            kernel,
            out_shape=pltpu.VMEM((total, 2 * LANES), BF16),
            in_specs=[SMEM] + [VMEM] * inputs,
            out_specs=VMEM,
            scratch_shapes=[pltpu.VMEM((rows, LANES), F32)],
            compiler_params=params(16),
            **more,
        )

    (taps,) = near_memory(conv_taps)
    inner = mixer(inner_kernel, 2, total + 16)(sink_logit, taps, *near_memory(full))
    mixed = mixer(outer, 5, 32, input_output_aliases={3: 0})(sink_logit, taps, *near_memory(full, inner, early, late))
    parts = lax.all_to_all(mixed.reshape(4, chunk, 2 * LANES), "tp", split_axis=0, concat_axis=0, tiled=True)
    step = 512
    steps = out_weight.shape[1] // step
    return pl.pallas_call(
        out_kernel,
        name="project_out",
        out_shape=jax.ShapeDtypeStruct((chunk, out_weight.shape[1]), BF16),
        in_specs=[VMEM] * 2,
        out_specs=pl.BlockSpec(memory_space=pltpu.HBM),
        scratch_shapes=[pltpu.VMEM((steps, chunk, step), BF16), pltpu.SemaphoreType.DMA((steps,))],
        compiler_params=params(16),
    )(*near_memory(parts, out_weight))


def solution(mesh):
    placed = (
        P(("sp", "tp"), None),
        P(),
        P(None, "tp"),
        P(None, "tp"),
        P(None, "tp"),
        P("tp"),
        P(None, "tp"),
        P(None, "tp"),
        P(None, "tp"),
        P(None, "tp"),
        P(),
    )

    return jax.shard_map(body, mesh=mesh, in_specs=placed, out_specs=P(("sp", "tp"), None), check_vma=False)
```

```python
import jax
import jax.numpy as jnp
from jax import lax
from jax.experimental import pallas as pl
from jax.experimental.pallas import tpu as pltpu
from jax.sharding import PartitionSpec as P


HEAD = 64
WIN = 128
EDGE = 16
LANES = 128
F32 = jnp.float32
BF16 = jnp.bfloat16
VMEM = pl.BlockSpec(memory_space=pltpu.VMEM)
SMEM = pl.BlockSpec(memory_space=pltpu.SMEM)


def near_memory(*arrays):
    return tuple(pltpu.with_memory_space_constraint(array, pltpu.VMEM) for array in arrays)


def params(mebibytes):
    return pltpu.CompilerParams(vmem_limit_bytes=mebibytes << 20)


def start_copies(pairs, sems):
    copies = [pltpu.make_async_copy(source, target, sems.at[i]) for i, (source, target) in enumerate(pairs)]
    for copy in copies:
        copy.start()
    return copies


def run_copies(pairs, sems):
    for copy in start_copies(pairs, sems):
        copy.wait()


def split_kernel(tokens_ref, gain_ref, top_ref, bottom_ref, gain_out_ref, sems):
    rows = top_ref.shape[0]
    run_copies(
        (
            (gain_ref, gain_out_ref),
            (tokens_ref.at[pl.ds(0, rows)], top_ref),
            (tokens_ref.at[pl.ds(rows, bottom_ref.shape[0])], bottom_ref),
        ),
        sems,
    )


def normalize(pieces, gain_ref, normed_ref):
    row = 0
    for ref in pieces:

        def strip(i, carry, ref=ref, row=row):
            at = pl.multiple_of(i * EDGE, EDGE)
            block = ref[pl.ds(at, EDGE), :].astype(F32)
            scale = lax.rsqrt(jnp.mean(block * block, axis=-1, keepdims=True) + 1e-06)
            normed_ref[pl.ds(pl.multiple_of(row + at, EDGE), EDGE), :] = (block * scale * gain_ref[...]).astype(BF16)
            return carry

        lax.fori_loop(0, ref.shape[0] // EDGE, strip, 0, unroll=True)
        row += ref.shape[0]


def project(normed_ref, cols_ref, rows_ref, full_ref, places):
    normed = normed_ref[...]
    out = jnp.dot(normed, cols_ref[...], preferred_element_type=F32).astype(BF16)
    pairs = lax.dot_general(normed, rows_ref[...], (((1,), (1,)), ((), ())), preferred_element_type=F32).astype(BF16)
    row = 0
    for start, count in places:
        part = out[row : row + count]
        product = part[:, 2 * LANES : 3 * LANES].astype(F32) * part[:, 3 * LANES :].astype(F32)
        where = pl.ds(pl.multiple_of(start, EDGE), count)
        full_ref[where, : 2 * LANES] = part[:, : 2 * LANES]
        full_ref[where, 2 * LANES : 3 * LANES] = product.astype(BF16)
        full_ref[where, 3 * LANES :] = pairs[row : row + count]
        row += count


def take_edge(full_ref, edge_ref, tail):
    total = full_ref.shape[0]
    pair = pl.multiple_of(jnp.where(tail, total - WIN, 0), EDGE)
    lane = lax.broadcasted_iota(jnp.int32, (WIN, LANES), 1)
    keys = full_ref[pl.ds(pair, WIN), 3 * LANES : 4 * LANES].astype(F32)
    values = full_ref[pl.ds(pair, WIN), 4 * LANES :].astype(F32)
    edge_ref[:WIN, :] = jnp.where(lane < HEAD, keys, values).astype(BF16)
    edge = pl.multiple_of(jnp.where(tail, total - EDGE, 0), EDGE)
    edge_ref[WIN:, :] = full_ref[pl.ds(edge, EDGE), 2 * LANES : 3 * LANES]


def near_kernel(*refs):
    *pieces, gain_ref = refs[:5]
    q_ref, k_ref, v_ref, gate_ref, pre_ref, input_ref = refs[5:11]
    full_ref, cols_ref, rows_ref, normed_ref, sems = refs[11:]
    pairs = [
        (ref, cols_ref.at[:, pl.ds(place * LANES, LANES)])
        for place, ref in enumerate((q_ref, gate_ref, pre_ref, input_ref))
    ]
    pairs += [
        (ref, rows_ref.at[pl.ds(place * HEAD, HEAD)]) for place, ref in enumerate((k_ref, k_ref, v_ref, v_ref))
    ]
    copies = start_copies(pairs, sems)
    normalize(pieces, gain_ref, normed_ref)
    for copy in copies:
        copy.wait()
    place = lax.axis_index("tp")
    chunk = full_ref.shape[0] // 4
    upper, lower = pieces[0].shape[0], pieces[1].shape[0]
    places = [(place * chunk, chunk), ((place ^ 1) * chunk, upper), ((place ^ 3) * chunk + upper, lower)]
    project(normed_ref, cols_ref, rows_ref, full_ref, places)


def middle_kernel(past_ref, a_ref, b_ref, gain_ref, cols_ref, rows_ref, full_ref, early_ref, normed_ref):
    normalize((a_ref, b_ref), gain_ref, normed_ref)
    place = lax.axis_index("tp")
    chunk = full_ref.shape[0] // 4
    lower, upper = a_ref.shape[0], b_ref.shape[0]
    places = [((place ^ 1) * chunk + upper, lower), ((place ^ 3) * chunk, upper)]
    project(normed_ref, cols_ref, rows_ref, full_ref, places)
    take_edge(full_ref, early_ref, place != 1)


def far_kernel(past_ref, top_ref, bottom_ref, gain_ref, cols_ref, rows_ref, full_ref, late_ref, normed_ref):
    normalize((top_ref, bottom_ref), gain_ref, normed_ref)
    place = lax.axis_index("tp")
    chunk = full_ref.shape[0] // 4
    project(normed_ref, cols_ref, rows_ref, full_ref, [((place ^ 2) * chunk, chunk)])
    take_edge(full_ref, late_ref, place == 1)


def attend(query, keys, values, sink, before, after):
    lane = lax.broadcasted_iota(jnp.int32, (WIN, LANES), 1)
    row = lax.rem(lax.broadcasted_iota(jnp.int32, (2 * WIN, WIN), 0), WIN)
    col = lax.broadcasted_iota(jnp.int32, (2 * WIN, WIN), 1)
    earlier, later = col >= row, col <= row
    if before is not None:
        earlier = earlier & before
    if after is not None:
        later = later & after
    scaled = query.astype(F32) * HEAD ** (-0.5)
    both = jnp.concatenate([jnp.where(lane < HEAD, scaled, 0.0), jnp.where(lane < HEAD, 0.0, scaled)], axis=0)
    score = lax.dot_general(both.astype(BF16), keys, (((1,), (1,)), ((), ())), preferred_element_type=F32)
    parts = (
        jnp.where(earlier, score[:, :WIN], -jnp.inf),
        score[:, WIN : 2 * WIN],
        jnp.where(later, score[:, 2 * WIN :], -jnp.inf),
    )
    most = jnp.maximum(jnp.maximum(parts[0], parts[1]), parts[2])
    top = jnp.maximum(jnp.max(most, axis=-1, keepdims=True), sink)
    expo = jnp.concatenate([jnp.exp(part - top).astype(BF16) for part in parts], axis=1)
    wide = jnp.concatenate([values, jnp.ones_like(values)], axis=1)
    got = jnp.dot(expo, wide, preferred_element_type=F32)
    denom = got[:, LANES:] + jnp.exp(sink - top)
    chosen = jnp.where(lane < HEAD, got[:WIN, :LANES], got[WIN:, :LANES])
    return (chosen / jnp.where(lane < HEAD, denom[:WIN], denom[WIN:])).astype(BF16)


def sink_column(sink_ref):
    half = lax.broadcasted_iota(jnp.int32, (2 * WIN, 1), 0) < WIN
    return jnp.where(half, sink_ref[0], sink_ref[1])


def convolve(taps_ref, conv_ref, count):
    return (
        taps_ref[0:1, :] * conv_ref[7 : 7 + count, :]
        + taps_ref[1:2, :] * conv_ref[8 : 8 + count, :]
        + taps_ref[2:3, :] * conv_ref[9 : 9 + count, :]
    )


def inner_kernel(sink_ref, taps_ref, full_ref, out_ref, conv_ref):
    total = full_ref.shape[0]
    conv_ref[0:8, :] = jnp.zeros((8, LANES), F32)
    conv_ref[8 : 8 + total, :] = full_ref[:, 2 * LANES : 3 * LANES].astype(F32)
    conv_ref[8 + total :, :] = jnp.zeros((8, LANES), F32)
    gate = full_ref[:, LANES : 2 * LANES].astype(F32)
    out_ref[:, LANES:] = (gate * convolve(taps_ref, conv_ref, total)).astype(BF16)
    sink = sink_column(sink_ref)
    for at in range(WIN, total - WIN, WIN):
        window = slice(at - WIN, at + 2 * WIN)
        out_ref[at : at + WIN, :LANES] = attend(
            full_ref[at : at + WIN, :LANES],
            full_ref[window, 3 * LANES : 4 * LANES],
            full_ref[window, 4 * LANES :],
            sink,
            None,
            None,
        )


def outer_kernel(sink_ref, taps_ref, full_ref, inner_ref, early_ref, late_ref, out_ref, conv_ref, *, last):
    total = full_ref.shape[0]
    place = lax.axis_index("sp")
    swapped = lax.axis_index("tp") == 1
    early, late = early_ref[...].astype(F32), late_ref[...].astype(F32)
    low, high = jnp.where(swapped, late, early), jnp.where(swapped, early, late)
    lane = lax.broadcasted_iota(jnp.int32, (WIN, LANES), 1)

    def unpack(halo):
        pair = halo[:WIN]
        turned = pltpu.roll(pair, HEAD, 1)
        keys, values = jnp.where(lane < HEAD, pair, turned), jnp.where(lane < HEAD, turned, pair)
        return keys.astype(BF16), values.astype(BF16)

    sink = sink_column(sink_ref)
    for at, halo in ((0, low), (total - WIN, high)):
        first = at == 0
        window = slice(0, 2 * WIN) if first else slice(total - 2 * WIN, total)
        sides = []
        for piece, lanes in zip(unpack(halo), (3, 4)):
            own = full_ref[window, lanes * LANES : (lanes + 1) * LANES]
            sides.append(jnp.concatenate([piece, own] if first else [own, piece], axis=0))
        out_ref[at : at + WIN, :LANES] = attend(
            full_ref[at : at + WIN, :LANES],
            *sides,
            sink,
            place != 0 if first else None,
            None if first else place != last,
        )
        if first:
            conv_ref[0:8, :] = halo[WIN + EDGE - 8 :]
            conv_ref[8:32, :] = full_ref[0:32, 2 * LANES : 3 * LANES].astype(F32)[:24]
        else:
            conv_ref[0:24, :] = full_ref[total - 32 :, 2 * LANES : 3 * LANES].astype(F32)[8:]
            conv_ref[24:32, :] = halo[WIN : WIN + 8]
        rows = slice(0, EDGE) if first else slice(total - EDGE, total)
        gate = full_ref[rows, LANES : 2 * LANES].astype(F32)
        out_ref[rows, LANES:] = (gate * convolve(taps_ref, conv_ref, EDGE)).astype(BF16)


def out_kernel(parts_ref, weight_ref, out_ref, done_ref, sems):
    count = parts_ref.shape[0]
    joined = jnp.concatenate(
        [parts_ref[i, :, :LANES] for i in range(count)] + [parts_ref[i, :, LANES:] for i in range(count)], axis=1
    )
    steps, _, step = done_ref.shape
    copies = []
    for i in range(steps):
        columns = pl.ds(i * step, step)
        done_ref[i] = jnp.dot(joined, weight_ref[:, columns], preferred_element_type=F32).astype(BF16)
        copies.append(pltpu.make_async_copy(done_ref.at[i], out_ref.at[:, columns], sems.at[i]))
        copies[-1].start()
    for copy in copies:
        copy.wait()


def body(
    tokens,
    norm_gain,
    query_weight,
    key_weight,
    value_weight,
    sink_logit,
    conv_gate_weight,
    conv_pre_weight,
    conv_input_weight,
    conv_taps,
    out_weight,
):
    chunk, width = tokens.shape
    total = 4 * chunk

    def local(kernel, shapes, count, **more):
        return pl.pallas_call(
            kernel,
            out_shape=tuple(pltpu.VMEM(shape, dtype) for shape, dtype in shapes),
            in_specs=[VMEM] * count,
            out_specs=(VMEM,) * len(shapes),
            compiler_params=params(16),
            **more,
        )

    def in_hbm(*arrays):
        return tuple(pltpu.with_memory_space_constraint(array, pltpu.HBM) for array in arrays)

    def loader(kernel, shapes, count):
        return pl.pallas_call(
            kernel,
            out_shape=tuple(pltpu.VMEM(shape, dtype) for shape, dtype in shapes),
            in_specs=[pl.BlockSpec(memory_space=pltpu.HBM)] * count,
            out_specs=(VMEM,) * len(shapes),
            scratch_shapes=[pltpu.SemaphoreType.DMA((9,))],
            compiler_params=params(16),
        )

    lead = chunk // 2 + EDGE
    top, bottom, gain = loader(
        split_kernel, (((lead, width), BF16), ((chunk - lead, width), BF16), ((1, width), F32)), 2
    )(*in_hbm(tokens, norm_gain.reshape(1, width)))

    def swap(block, turn):
        return lax.ppermute(block, "tp", [(i, i ^ turn) for i in range(4)])

    a_top = swap(top, 1)
    b_bottom = swap(bottom, 3)
    a_bottom = swap(bottom, 1)
    b_top = swap(top, 3)
    far_top = swap(a_top, 3)
    far_bottom = swap(b_bottom, 1)

    full_shape = ((total, 5 * LANES), BF16)
    edge_shape = ((WIN + EDGE, LANES), BF16)
    near_shapes = (full_shape, ((width, 4 * LANES), BF16), ((2 * LANES, width), BF16))
    full, cols, rows = pl.pallas_call(
        near_kernel,
        name="near",
        out_shape=tuple(pltpu.VMEM(shape, dtype) for shape, dtype in near_shapes),
        in_specs=[VMEM] * 5 + [pl.BlockSpec(memory_space=pltpu.HBM)] * 6,
        out_specs=(VMEM,) * 3,
        scratch_shapes=[pltpu.VMEM((2 * chunk, width), BF16), pltpu.SemaphoreType.DMA((8,))],
        compiler_params=params(16),
    )(
        *near_memory(top, bottom, a_top, b_bottom, gain),
        *in_hbm(query_weight, key_weight.T, value_weight.T, conv_gate_weight, conv_pre_weight, conv_input_weight),
    )
    weights = (gain, cols, rows)
    more = {"input_output_aliases": {0: 0}, "scratch_shapes": [pltpu.VMEM((chunk, width), BF16)]}
    full, early = local(middle_kernel, (full_shape, edge_shape), 6, **more)(
        *near_memory(full, a_bottom, b_top, *weights)
    )
    count = lax.axis_size("sp")
    ups = {x: [(4 * i + x, 4 * i + 4 + x) for i in range(count - 1)] for x in range(4)}
    downs = {x: [(j, i) for i, j in pairs] for x, pairs in ups.items()}
    early = lax.ppermute(early, ("sp", "tp"), ups[0] + downs[1] + ups[2] + ups[3])
    full, late = local(far_kernel, (full_shape, edge_shape), 6, **more)(
        *near_memory(full, far_top, far_bottom, *weights)
    )
    late = lax.ppermute(late, ("sp", "tp"), downs[0] + ups[1] + downs[2] + downs[3])

    def outer(*refs):
        outer_kernel(*refs, last=count - 1)

    (taps,) = near_memory(conv_taps)
    mixed_shape = (total, 2 * LANES)
    inner = pl.pallas_call(
        inner_kernel,
        name="inner",
        out_shape=pltpu.VMEM(mixed_shape, BF16),
        in_specs=[SMEM] + [VMEM] * 2,
        out_specs=VMEM,
        scratch_shapes=[pltpu.VMEM((total + 16, LANES), F32)],
        compiler_params=params(16),
    )(sink_logit, taps, *near_memory(full))
    mixed = pl.pallas_call(
        outer,
        name="outer",
        out_shape=pltpu.VMEM(mixed_shape, BF16),
        in_specs=[SMEM] + [VMEM] * 5,
        out_specs=VMEM,
        scratch_shapes=[pltpu.VMEM((32, LANES), F32)],
        compiler_params=params(16),
        input_output_aliases={3: 0},
    )(sink_logit, taps, *near_memory(full, inner, early, late))
    parts = lax.all_to_all(mixed.reshape(4, chunk, 2 * LANES), "tp", split_axis=0, concat_axis=0, tiled=True)
    step = 512
    steps = out_weight.shape[1] // step
    return pl.pallas_call(
        out_kernel,
        name="project_out",
        out_shape=jax.ShapeDtypeStruct((chunk, out_weight.shape[1]), BF16),
        in_specs=[VMEM] * 2,
        out_specs=pl.BlockSpec(memory_space=pltpu.HBM),
        scratch_shapes=[pltpu.VMEM((steps, chunk, step), BF16), pltpu.SemaphoreType.DMA((steps,))],
        compiler_params=params(16),
    )(*near_memory(parts, out_weight))


def solution(mesh):
    placed = (
        P(("sp", "tp"), None),
        P(),
        P(None, "tp"),
        P(None, "tp"),
        P(None, "tp"),
        P("tp"),
        P(None, "tp"),
        P(None, "tp"),
        P(None, "tp"),
        P(None, "tp"),
        P(),
    )

    return jax.shard_map(body, mesh=mesh, in_specs=placed, out_specs=P(("sp", "tp"), None), check_vma=False)
```
